512 devices in a mesh: ep: 32 (over z, core), tp: 16 (over y, x).
Axes of the slice: x: 4, y: 4, z: 16, core: 2. Of those that a mesh axis runs over, the one named last changes fastest.
Arguments:
- tokens: bfloat16 [1024, 2048], P('ep', 'tp'), may hold values from -200 to 200
- routing: int32 [1024, 4], P('ep'), may hold values from 0 to 63, all different within a row; in each aligned block of 32 rows (0 to 31, 32 to 63, ...) at most 8 rows name the same one
- gate_weights: float32 [1024, 4], P('ep'), may hold values from 0.05 to 1
- norm_gain: float32 [2048], replicated, may hold values from 0.1 to 1.9
- w_gate: bfloat16 [64, 2048, 2048], P('ep', None, 'tp'), may hold values from -0.33007812 to 0.33007812
- w_up: bfloat16 [64, 2048, 2048], P('ep', None, 'tp'), may hold values from -0.33007812 to 0.33007812
- w_down: bfloat16 [64, 2048, 2048], P('ep', 'tp'), may hold values from -0.026489258 to 0.026489258
Outputs:
- mixed: bfloat16 [1024, 2048], P('ep', 'tp')
The draws below stay inside these ranges and needn't reach their ends.
Inputs may be any that keep to these rules, and one draw needn't show every extreme that they name: `routing`: each token names 4 different experts. Among the 32 tokens of one index of ep no expert is named more than 8 times, a bound that some block reaches.
All inputs are finite; a program needn't handle non-finite values.
Results may differ from the reference program's by a relative error of at most 0.015.
Values may be sent and summed in bfloat16 or wider, within the bound.
A program may use at most 128 MiB of HBM per device.

```python
import math
import jax
import jax.numpy as jnp
import numpy as np
from jax import lax

D = 2048
FF = 2048
TOP = 4
EXP_DEV = 2
TOK_DEV = 32
CAP = 8
EXPERTS = 64
TOKENS = 1024
N_EP = 32
N_TP = 16


def draw_tokens(key, part):
    base_key, scale_key, row_key, mean_key = jax.random.split(key, 4)
    values = jax.random.normal(base_key, (TOKENS, D), jnp.float32)
    values = jnp.clip(values, -6.0, 6.0)
    column_scale = jnp.exp(jax.random.uniform(scale_key, (D // 16,), jnp.float32, jnp.log(0.3), jnp.log(3.0)))
    values = values * jnp.repeat(column_scale, 16)[None, :]
    return values.astype(jnp.bfloat16)


def block_levels(stream_key, dims, cuts, smallest, top_value):
    loudness = 1.0
    for axis_at, shards_of in cuts:
        draws = jax.random.uniform(jax.random.fold_in(jax.random.fold_in(stream_key, 6), axis_at), (shards_of,), jnp.float32, smallest / len(cuts), top_value / len(cuts))
        loudness = loudness * jnp.repeat(jnp.exp(draws), dims[axis_at] // shards_of).reshape((-1,) + (1,) * (len(dims) - 1 - axis_at))
    return loudness


def routed_block(key, own, number, rows, count, top, most, skew):
    order = jax.random.permutation(key, count)
    crowded, common = load_shares(count, rows * top, most, skew, True), load_shares(count, rows * top, most, skew, False)
    places = jnp.arange(count)

    def named(lengths, rotation):
        used = int((lengths > 0).sum())
        fixed = max(1, used // 4)
        moved = fixed + (places - fixed + rotation * (used - fixed)) % max(1, count - fixed)
        return jnp.zeros((count,), jnp.int32).at[order[jnp.where(places < fixed, places, moved)]].set(jnp.asarray(lengths, jnp.int32))

    lengths = jnp.where(number % 4 == 0, named(crowded, number // 4), named(common, number - number // 4 - 1))
    mixed = jax.random.permutation(jax.random.fold_in(own, 3), count)
    giver, taker = mixed[0:count // 2 * 2:2], mixed[1:count // 2 * 2:2]
    room = jnp.minimum(lengths[giver] - 1, most - lengths[taker]) // 2
    room = jnp.where((giver == order[0]) | (taker == order[0]) | (lengths[taker] == 0), 0, jnp.maximum(room, 0))
    moved = jax.random.randint(jax.random.fold_in(own, 4), (count // 2,), 0, 1 << 20) % (room + 1)
    lengths = lengths.at[giver].add(-moved).at[taker].add(moved)
    members = jnp.searchsorted(jnp.cumsum(lengths), jnp.arange(rows * top), side="right").astype(jnp.int32)
    listing = members.reshape(top, rows).T
    listing = listing[jax.random.permutation(jax.random.fold_in(own, 1), rows)]
    rotation = jax.random.randint(jax.random.fold_in(own, 2), (rows, 1), 0, top)
    return jnp.take_along_axis(listing, (jnp.arange(top)[None, :] + rotation) % top, axis=1)


def load_shares(amount, total, most, slope, full):
    weights = [(1 << 20) // math.isqrt(grade ** slope) + 1 for grade in range(1, amount + 1)]
    largest = most if full else min(most, max(-(-total // amount), total * weights[0] // sum(weights)))
    least = 1 if total - largest >= amount - 1 else 0
    counts, rest = [largest] + [least] * (amount - 1), total - largest - least * (amount - 1)
    while rest > 0:
        free = [i for i in range(1, amount) if counts[i] < largest] or [i for i in range(1, amount) if counts[i] < most]
        whole, left = sum([weights[i] for i in free]), rest
        for i in free:
            more = min(most - counts[i], max(1, left * weights[i] // whole), rest)
            counts[i] = counts[i] + more
            rest = rest - more
    return np.array(counts)


def scatter_about(key, shape, deviation, reach, pieces=(), held_as=jnp.bfloat16):
    drawn = deviation * jax.random.normal(key, shape, jnp.float32)
    if pieces:
        drawn = drawn * block_levels(key, shape, pieces, -0.22, 0.18)
    return jnp.clip(drawn, -reach, reach).astype(held_as)


def setup_inputs(seed: int = 0) -> dict:
    keys = jax.random.split(jax.random.key(seed), 8)
    tokens = draw_tokens(jax.random.fold_in(keys[7], 71), 0)
    routing_keys = jax.random.split(jax.random.fold_in(keys[1], 1), TOKENS // TOK_DEV)
    routing_turns = jax.random.permutation(jax.random.fold_in(keys[1], 3), TOKENS // TOK_DEV)
    routing = jax.vmap(lambda own, number: routed_block(jax.random.fold_in(keys[1], 2), own, number, TOK_DEV, EXP_DEV * N_EP, TOP, CAP, 2))(routing_keys, routing_turns).reshape((TOKENS, TOP))
    gate_weights = jnp.clip(jnp.exp(math.log(1.0) - 2.9957323 * jax.random.uniform(keys[2], (TOKENS, TOP), jnp.float32) ** block_levels(keys[2], (TOKENS, TOP), ((0, 32),), -0.2, 0.2)), 0.05, 1.0)
    norm_gain = jnp.clip(1.0 + 0.18 * jax.random.normal(keys[3], (D,), jnp.float32), 0.1, 1.9)
    w_gate = scatter_about(keys[4], (EXPERTS, D, FF), (2.5 * D ** -0.5), 0.33007812, ((0, 32), (2, 16)))
    w_up = scatter_about(keys[5], (EXPERTS, D, FF), (2.5 * D ** -0.5), 0.33007812, ((0, 32), (2, 16)))
    w_down = scatter_about(keys[6], (EXPERTS, FF, D), (0.2 * FF ** -0.5), 0.026489258, ((0, 32), (1, 16)))
    return dict(tokens=tokens, routing=routing, gate_weights=gate_weights, norm_gain=norm_gain, w_gate=w_gate, w_up=w_up, w_down=w_down)


norm_eps = 1e-06
clamp_limit = 7.0
swish_alpha = 1.702

def expert_apply(inputs):
    rows, gate_mat, up_mat, down_mat = inputs
    pre_gate = jnp.dot(rows, gate_mat, preferred_element_type=jnp.float32)
    pre_up = jnp.dot(rows, up_mat, preferred_element_type=jnp.float32)
    clamped = jnp.minimum(pre_gate, clamp_limit)
    upper = jnp.clip(pre_up, -clamp_limit, clamp_limit)
    hidden = (clamped * jax.nn.sigmoid(swish_alpha * clamped) * (upper + 1.0)).astype(jnp.bfloat16)
    block_width = FF // N_TP
    hidden_blocks = hidden.reshape(hidden.shape[0], N_TP, block_width).astype(jnp.float32)
    down_blocks = down_mat.reshape(N_TP, block_width, D).astype(jnp.float32)
    partial_value = jnp.einsum('rnf,nfd->nrd', hidden_blocks, down_blocks)
    rounded = partial_value.astype(jnp.bfloat16).astype(jnp.float32)
    return lax.optimization_barrier(jnp.sum(rounded, axis=0)).astype(jnp.bfloat16)

def reference(tokens, routing, gate_weights, norm_gain, w_gate, w_up, w_down):
    expert_count = EXP_DEV * N_EP
    wide = tokens.astype(jnp.float32)
    ssq = lax.optimization_barrier(jnp.sum(wide * wide, axis=1, keepdims=True))
    normed = (wide * lax.rsqrt(ssq / D + norm_eps) * norm_gain[None, :]).astype(jnp.bfloat16)
    grouped = routing.reshape(N_EP, TOK_DEV * TOP)
    onehot = (grouped[:, :, None] == jnp.arange(expert_count, dtype=jnp.int32)[None, None, :]).astype(jnp.int32)
    slot_rank = lax.optimization_barrier(jnp.sum(jnp.cumsum(onehot, axis=1) * onehot, axis=2)) - 1
    groups = jnp.arange(N_EP, dtype=jnp.int32)[:, None]
    slot_index = (grouped * (N_EP * CAP) + groups * CAP + slot_rank).reshape(-1).astype(jnp.int32)
    repeated = jnp.repeat(normed, TOP, axis=0)
    buffer = jnp.zeros((expert_count * N_EP * CAP, D), jnp.bfloat16).at[slot_index].set(repeated)
    buffer = buffer.reshape(expert_count, N_EP * CAP, D)
    expert_out = lax.map(expert_apply, (buffer, w_gate, w_up, w_down))
    picked = expert_out.reshape(-1, D)[slot_index].astype(jnp.float32).reshape(TOKENS, TOP, D)
    mixed = lax.optimization_barrier(jnp.sum(gate_weights[:, :, None] * picked, axis=1))
    return mixed.astype(jnp.bfloat16)
```

```python
import jax
import jax.numpy as jnp
from jax import lax
from jax.sharding import PartitionSpec as P

D = 2048
CAP = 8

norm_eps = 1e-06
clamp_limit = 7.0
swish_alpha = 1.702


def activate(pre_gate, pre_up):
    clamped = jnp.minimum(pre_gate, clamp_limit)
    upper = jnp.clip(pre_up, -clamp_limit, clamp_limit)
    return (clamped * jax.nn.sigmoid(swish_alpha * clamped) * (upper + 1.0)).astype(jnp.bfloat16)


def per_device(tokens, routing, gate_weights, norm_gain, w_gate, w_up, w_down):
    ep_size = lax.axis_size("ep")
    exp_here = w_gate.shape[0]
    expert_count = exp_here * ep_size
    tok_rows = tokens.shape[0]
    top_count = routing.shape[1]
    col_width = tokens.shape[1]
    chosen = routing.reshape(-1)
    onehot = (chosen[:, None] == jnp.arange(expert_count, dtype=jnp.int32)[None, :]).astype(
        jnp.int32
    )
    slot_rank = jnp.sum(jnp.cumsum(onehot, axis=0) * onehot, axis=1) - 1
    slot_index = (chosen * CAP + slot_rank).reshape(tok_rows, top_count)
    slot_ids = jnp.arange(expert_count * CAP, dtype=jnp.int32)
    matches = slot_ids[:, None, None] == slot_index[None, :, :]
    placing = jnp.sum(matches.astype(jnp.float32), axis=2).astype(jnp.bfloat16)
    outgoing = jnp.dot(placing, tokens, preferred_element_type=jnp.float32).astype(jnp.bfloat16)
    outgoing = outgoing.reshape(ep_size, exp_here, CAP, col_width)
    received = lax.all_to_all(outgoing, "ep", split_axis=0, concat_axis=0, tiled=True)
    received = jnp.transpose(received, (1, 0, 2, 3)).reshape(exp_here, ep_size * CAP, col_width)
    raw = lax.all_gather(received, "tp", axis=2, tiled=True)
    wide = raw.astype(jnp.float32)
    ssq = jnp.sum(wide * wide, axis=2, keepdims=True)
    rows = (wide * lax.rsqrt(ssq / D + norm_eps) * norm_gain).astype(jnp.bfloat16)
    gate_part = jnp.einsum("erd,edf->erf", rows, w_gate, preferred_element_type=jnp.float32)
    up_part = jnp.einsum("erd,edf->erf", rows, w_up, preferred_element_type=jnp.float32)
    hidden = activate(gate_part, up_part)
    partial_value = jnp.einsum("erf,efd->erd", hidden, w_down, preferred_element_type=jnp.float32)
    summed = lax.psum_scatter(
        partial_value.astype(jnp.bfloat16), "tp", scatter_dimension=2, tiled=True
    )
    summed = jnp.transpose(summed.reshape(exp_here, ep_size, CAP, col_width), (1, 0, 2, 3))
    returned = lax.all_to_all(summed, "ep", split_axis=0, concat_axis=0, tiled=True)
    returned = returned.reshape(expert_count * CAP, col_width).astype(jnp.float32)
    combine = jnp.sum(matches.astype(jnp.float32) * gate_weights[None, :, :], axis=2)
    mixed = jnp.dot(combine.T, returned, precision=lax.Precision.HIGHEST)
    return mixed.astype(jnp.bfloat16)


def solution(mesh):
    placed = (
        P("ep", "tp"),
        P("ep", None),
        P("ep", None),
        P(),
        P("ep", None, "tp"),
        P("ep", None, "tp"),
        P("ep", "tp", None),
    )
    return jax.shard_map(
        per_device, mesh=mesh, in_specs=placed, out_specs=P("ep", "tp"), check_vma=False
    )
```

```python
import functools

import jax
import jax.numpy as jnp
from jax import lax
from jax.experimental import pallas as pl
from jax.experimental.pallas import tpu as pltpu
from jax.sharding import PartitionSpec as P

D = 2048
CAP = 8
NX = 4
NY = 4
NZ = 16
EXP_DEV = 2
LANES = 128
NC = 4
ORDER = (0, 1, -1, 2, -2, 3, -3, 4, -4, 5, -5, 6, -6, 7, -7, 8)
PER = NZ // NC
ROWS = PER * 2 * CAP
HALF = ROWS // 2

norm_eps = 1e-06
clamp_limit = 7.0
swish_alpha = 1.702
MESH = pl.DeviceIdType.MESH


def activate(pre_gate, pre_up):
    clamped = jnp.minimum(pre_gate, clamp_limit)
    upper = jnp.clip(pre_up, -clamp_limit, clamp_limit)
    return (clamped * jax.nn.sigmoid(swish_alpha * clamped) * (upper + 1.0)).astype(jnp.bfloat16)


def kernel(
    tok, rout, gw, gain, wg, wu, wd, out,
    outgoing, gath, part, rb1, rb2, quart, rb3, rb4, final, ret, wgu, wdn, comb,
    wsem, zs, zr, rs, rr, hs, hr,
):
    ep = lax.axis_index("ep")
    tp = lax.axis_index("tp")
    z, core = ep // 2, lax.rem(ep, 2)
    y, x = tp // NX, lax.rem(tp, NX)

    def ring(value, step, size):
        return lax.rem(value + step + size, size)

    def ep_at(dz, other):
        return ring(z, dz, NZ) * 2 + (lax.rem(core + other, 2))

    def beside(axis, step):
        if axis == "x":
            return {"tp": y * NX + ring(x, step, NX)}
        return {"tp": ring(y, step, NY) * NX + x}

    weights = [
        pltpu.make_async_copy(wg, wgu.at[:, :, pl.ds(0, LANES)], wsem.at[0]),
        pltpu.make_async_copy(wu, wgu.at[:, :, pl.ds(LANES, LANES)], wsem.at[1]),
        pltpu.make_async_copy(wd, wdn, wsem.at[2]),
    ]
    for copy in weights:
        copy.start()

    barrier = pltpu.get_barrier_semaphore()
    peers = [{"ep": ep_at(d, o)} for d in ORDER for o in range(2) if (d, o) != (0, 0)]
    peers += [beside(a, s) for a in ("x", "y") for s in (1, -1)]
    for peer in peers:
        pl.semaphore_signal(barrier, inc=1, device_id=peer, device_id_type=MESH)

    chosen = rout[...]
    lanes = lax.broadcasted_iota(jnp.int32, (32, 64), 1)
    hot = [jnp.where(chosen[:, k : k + 1] == lanes, 1.0, 0.0) for k in range(4)]
    named = hot[0] + hot[1] + hot[2] + hot[3]
    lower = jnp.where(
        lax.broadcasted_iota(jnp.int32, (32, 32), 0) > lax.broadcasted_iota(jnp.int32, (32, 32), 1),
        1.0, 0.0,
    )
    before = jnp.dot(
        lower.astype(jnp.bfloat16), named.astype(jnp.bfloat16), preferred_element_type=jnp.float32
    )
    slots = lax.broadcasted_iota(jnp.int32, (32, 512), 1)
    place = jnp.zeros((32, 512), jnp.float32)
    mix = jnp.zeros((32, 512), jnp.float32)
    for k in range(4):
        rank = jnp.sum(before * hot[k], axis=1, keepdims=True).astype(jnp.int32)
        match = (chosen[:, k : k + 1] * CAP + rank) == slots
        place = place + jnp.where(match, 1.0, 0.0)
        mix = mix + jnp.where(match, gw[:, k : k + 1], 0.0)
    comb[...] = mix
    outgoing[...] = lax.dot_general(
        place.astype(jnp.bfloat16), tok[...], (((0,), (0,)), ((), ())),
        preferred_element_type=jnp.float32,
    ).astype(jnp.bfloat16).reshape(32, EXP_DEV, CAP, LANES)

    pl.semaphore_wait(barrier, len(peers))

    sends = []

    def send(src, dst, ssem, rsem, device):
        copy = pltpu.make_async_remote_copy(
            src_ref=src, dst_ref=dst, send_sem=ssem, recv_sem=rsem, device_id=device,
            device_id_type=MESH,
        )
        copy.start()
        sends.append(copy)
        return copy

    place_of = {}
    for i, d in enumerate(ORDER):
        place_of[d % NZ] = (i // PER, i % PER)

    zcopies = {}
    for i, d in enumerate(ORDER):
        for o in range(2):
            c, k = place_of[(-d) % NZ]
            target = ep_at(d, o)
            where = 2 * k + o
            if (d, o) == (0, 0):
                own = outgoing[target]
                for e in range(EXP_DEV):
                    gath[c, y, x, e, where] = own[e]
                continue
            zcopies[(c, where)] = send(
                outgoing.at[target], gath.at[c, y, x, :, where],
                zs.at[c * 2 * PER + where], zr.at[c * 2 * PER + where], {"ep": target},
            )

    live = {}
    first, second = ("x", "y"), ("y", "x")

    def pos(axis):
        return x if axis == "x" else y

    def hop(name, c, h, axis, views):
        stage = ("a1", "a2", "a3", "a4", "r1", "r2", "r3", "r4").index(name)
        made = []
        for j, step in enumerate((1, -1)):
            src, dst = views[j]
            idx = ((stage * NC + c) * 2 + h) * 2 + j
            made.append(send(src, dst, rs.at[idx], rr.at[idx], beside(axis, step)))
        live[(name, c, h)] = made

    def landed(name, c, h):
        for copy in live[(name, c, h)]:
            copy.wait_recv()

    def block(c, h, i, j, lo=0, n=ROWS // CAP):
        return gath.at[c, i, j, h, pl.ds(lo, n)]

    def line(ref, c, h, axis, at, lo=0, n=ROWS // CAP):
        if axis == "y":
            return ref.at[c, at, :, h, pl.ds(lo, n)]
        return ref.at[c, :, at, h, pl.ds(lo, n)]

    K2 = HALF // CAP

    def s0(c):
        for key, copy in zcopies.items():
            if key[0] == c:
                copy.wait_recv()
        for h in range(2):
            view = block(c, h, y, x)
            hop("a1", c, h, first[h], [(view, view)] * 2)

    def s1(c):
        for h in range(2):
            landed("a1", c, h)
            a = first[h]
            back, ahead = ring(pos(a), -1, 4), ring(pos(a), 1, 4)
            if a == "x":
                v0, v1 = block(c, h, y, back, 0, K2), block(c, h, y, ahead, K2, K2)
            else:
                v0, v1 = block(c, h, back, x, 0, K2), block(c, h, ahead, x, K2, K2)
            hop("a2", c, h, a, [(v0, v0), (v1, v1)])

    def s2(c):
        for h in range(2):
            landed("a2", c, h)
            a = second[h]
            view = line(gath, c, h, a, pos(a))
            hop("a3", c, h, a, [(view, view)] * 2)

    def s3(c):
        for h in range(2):
            landed("a3", c, h)
            a = second[h]
            v0 = line(gath, c, h, a, ring(pos(a), -1, 4), 0, K2)
            v1 = line(gath, c, h, a, ring(pos(a), 1, 4), K2, K2)
            hop("a4", c, h, a, [(v0, v0), (v1, v1)])

    def s4(c):
        for h in range(2):
            landed("a4", c, h)
            if c == 0 and h == 0:
                for copy in weights:
                    copy.wait()
            raw = jnp.concatenate(
                [gath[c, i, j, h].reshape(ROWS, LANES) for i in range(NY) for j in range(NX)],
                axis=1,
            )
            wide = raw.astype(jnp.float32)
            ssq = jnp.sum(wide * wide, axis=1, keepdims=True)
            rows = (wide * lax.rsqrt(ssq / D + norm_eps) * gain[...]).astype(jnp.bfloat16)
            both = jnp.dot(rows, wgu[h], preferred_element_type=jnp.float32)
            hidden = activate(both[:, :LANES], both[:, LANES:])
            value = jnp.dot(hidden, wdn[h], preferred_element_type=jnp.float32).astype(jnp.bfloat16)
            for i in range(NY):
                for j in range(NX):
                    at = (i * NX + j) * LANES
                    part[c, i, j, h] = value[:, at : at + LANES].reshape(ROWS // CAP, CAP, LANES)
            a = second[h]
            far = ring(pos(a), 2, 4)
            hop("r1", c, h, a, [
                (line(part, c, h, a, far, 0, K2), rb1.at[c, h, 0]),
                (line(part, c, h, a, far, K2, K2), rb1.at[c, h, 1]),
            ])

    def add_into(ref_view, other):
        ref_view[...] = (
            ref_view[...].astype(jnp.float32) + other[...].astype(jnp.float32)
        ).astype(jnp.bfloat16)

    def s5(c):
        for h in range(2):
            landed("r1", c, h)
            a = second[h]
            ahead, back = ring(pos(a), 1, 4), ring(pos(a), -1, 4)
            add_into(line(part, c, h, a, ahead, 0, K2), rb1.at[c, h, 0])
            add_into(line(part, c, h, a, back, K2, K2), rb1.at[c, h, 1])
            hop("r2", c, h, a, [
                (line(part, c, h, a, ahead), rb2.at[c, h, 0]),
                (line(part, c, h, a, back), rb2.at[c, h, 1]),
            ])

    def s6(c):
        for h in range(2):
            landed("r2", c, h)
            a, b = second[h], first[h]
            total = line(part, c, h, a, pos(a))[...].astype(jnp.float32)
            total = total + rb2[c, h, 0].astype(jnp.float32) + rb2[c, h, 1].astype(jnp.float32)
            quart[c, h] = total.astype(jnp.bfloat16)
            far = ring(pos(b), 2, 4)
            hop("r3", c, h, b, [
                (quart.at[c, h, far, pl.ds(0, K2)], rb3.at[c, h, 0]),
                (quart.at[c, h, far, pl.ds(K2, K2)], rb3.at[c, h, 1]),
            ])

    def s7(c):
        for h in range(2):
            landed("r3", c, h)
            b = first[h]
            ahead, back = ring(pos(b), 1, 4), ring(pos(b), -1, 4)
            add_into(quart.at[c, h, ahead, pl.ds(0, K2)], rb3.at[c, h, 0])
            add_into(quart.at[c, h, back, pl.ds(K2, K2)], rb3.at[c, h, 1])
            hop("r4", c, h, b, [
                (quart.at[c, h, ahead], rb4.at[c, h, 0]),
                (quart.at[c, h, back], rb4.at[c, h, 1]),
            ])

    homes = []

    def s8(c):
        for h in range(2):
            landed("r4", c, h)
            b = first[h]
            total = quart[c, h, pos(b)].astype(jnp.float32)
            total = total + rb4[c, h, 0].astype(jnp.float32) + rb4[c, h, 1].astype(jnp.float32)
            final[c, h] = total.astype(jnp.bfloat16)
        for k in range(PER):
            d = ORDER[c * PER + k]
            for o in range(2):
                where = 2 * k + o
                if (d, o) == (0, 0):
                    for e in range(EXP_DEV):
                        ret[ep, e] = final[c, e, where]
                    continue
                i = (c * PER + k) * 2 + o
                homes.append(
                    send(
                        final.at[c, :, where], ret.at[ep],
                        hs.at[i], hr.at[i], {"ep": ep_at(d, o)},
                    )
                )

    stages = (s0, s1, s2, s3, s4, s5, s6, s7, s8)
    for t in range(len(stages) + NC - 1):
        for c in range(NC):
            if 0 <= t - c < len(stages):
                stages[t - c](c)

    for copy in homes:
        copy.wait_recv()
    mixed = jnp.dot(
        comb[...], ret[...].reshape(512, LANES).astype(jnp.float32),
        preferred_element_type=jnp.float32, precision=lax.Precision.HIGHEST,
    )
    out[...] = mixed.astype(jnp.bfloat16)
    for copy in sends:
        copy.wait_send()


def per_device(tokens, routing, gate_weights, norm_gain, w_gate, w_up, w_down):
    vmem = pl.BlockSpec(memory_space=pltpu.VMEM)
    hbm = pl.BlockSpec(memory_space=pl.ANY)
    tiles = ROWS // CAP
    bf = jnp.bfloat16
    hops = 8 * NC * 2 * 2
    return pl.pallas_call(
        kernel,
        out_shape=jax.ShapeDtypeStruct((32, LANES), bf),
        in_specs=[vmem, vmem, vmem, vmem, hbm, hbm, hbm],
        out_specs=vmem,
        scratch_shapes=[
            pltpu.VMEM((32, EXP_DEV, CAP, LANES), bf),
            pltpu.VMEM((NC, NY, NX, EXP_DEV, tiles, CAP, LANES), bf),
            pltpu.VMEM((NC, NY, NX, EXP_DEV, tiles, CAP, LANES), bf),
            pltpu.VMEM((NC, 2, 2, 4, tiles // 2, CAP, LANES), bf),
            pltpu.VMEM((NC, 2, 2, 4, tiles, CAP, LANES), bf),
            pltpu.VMEM((NC, 2, 4, tiles, CAP, LANES), bf),
            pltpu.VMEM((NC, 2, 2, tiles // 2, CAP, LANES), bf),
            pltpu.VMEM((NC, 2, 2, tiles, CAP, LANES), bf),
            pltpu.VMEM((NC, 2, tiles, CAP, LANES), bf),
            pltpu.VMEM((32, EXP_DEV, CAP, LANES), bf),
            pltpu.VMEM((EXP_DEV, D, 2 * LANES), bf),
            pltpu.VMEM((EXP_DEV, LANES, D), bf),
            pltpu.VMEM((32, 512), jnp.float32),
            pltpu.SemaphoreType.DMA((3,)),
            pltpu.SemaphoreType.DMA((32,)),
            pltpu.SemaphoreType.DMA((32,)),
            pltpu.SemaphoreType.DMA((hops,)),
            pltpu.SemaphoreType.DMA((hops,)),
            pltpu.SemaphoreType.DMA((32,)),
            pltpu.SemaphoreType.DMA((32,)),
        ],
        compiler_params=pltpu.CompilerParams(
            collective_id=0, has_side_effects=True, vmem_limit_bytes=48 * 1024 * 1024
        ),
        name="moe_step",
    )(tokens, routing, gate_weights, norm_gain.reshape(1, D), w_gate, w_up, w_down)


def solution(mesh):
    placed = (
        P("ep", "tp"),
        P("ep", None),
        P("ep", None),
        P(),
        P("ep", None, "tp"),
        P("ep", None, "tp"),
        P("ep", "tp", None),
    )
    return jax.shard_map(
        per_device, mesh=mesh, in_specs=placed, out_specs=P("ep", "tp"), check_vma=False
    )
```

```python
import functools

import jax
import jax.numpy as jnp
from jax import lax
from jax.experimental import pallas as pl
from jax.experimental.pallas import tpu as pltpu
from jax.sharding import PartitionSpec as P

D = 2048
CAP = 8
NX = 4
NY = 4
NZ = 16
EXP_DEV = 2
LANES = 128
NC = 2
ORDER = (8, -7, 7, -6, 6, -5, 5, -4, 4, -3, 3, -2, 2, -1, 1, 0)
PER = NZ // NC
ROWS = PER * 2 * CAP
HALF = ROWS // 2

PLAN = (
    ("a1", 0, 0),
    ("a1", 0, 1),
    ("a3", 0, 0),
    ("a3", 0, 1),
    ("a1", 1, 0),
    ("a1", 1, 1),
    ("a4", 0, 0),
    ("a4", 0, 1),
    ("a3", 1, 1),
    ("a3", 1, 0),
    ("r1", 0, 0),
    ("r1", 0, 1),
    ("a4", 1, 1),
    ("a4", 1, 0),
    ("r2", 0, 0),
    ("r2", 0, 1),
    ("r1", 1, 0),
    ("r1", 1, 1),
    ("r3", 0, 0),
    ("r3", 0, 1),
    ("r2", 1, 0),
    ("r2", 1, 1),
    ("fin", 0, 0),
    ("fin", 0, 1),
    ("r3", 1, 0),
    ("r3", 1, 1),
    ("fin", 1, 0),
    ("fin", 1, 1),
)
WEIGHTS_AT = (0, 0)
GOES = ((0, 1), (1, 1))

norm_eps = 1e-06
clamp_limit = 7.0
swish_alpha = 1.702
MESH = pl.DeviceIdType.MESH


def activate(pre_gate, pre_up):
    clamped = jnp.minimum(pre_gate, clamp_limit)
    upper = jnp.clip(pre_up, -clamp_limit, clamp_limit)
    return (clamped * jax.nn.sigmoid(swish_alpha * clamped) * (upper + 1.0)).astype(jnp.bfloat16)


def kernel(
    tok_in, rout_in, gw_in, gain_in, wg, wu, wd, out,
    tok, rout, gw, gain, outgoing, gath, part, rb1, rb2, quart, rb4, final, ret, wgu, wdn, comb,
    wsem, zs, zr, rs, rr, hs, hr,
):
    ep = lax.axis_index("ep")
    tp = lax.axis_index("tp")
    z, core = ep // 2, lax.rem(ep, 2)
    y, x = tp // NX, lax.rem(tp, NX)

    def ring(value, step, size):
        return lax.rem(value + step + size, size)

    def ep_at(dz, other):
        return ring(z, dz, NZ) * 2 + (lax.rem(core + other, 2))

    def beside(axis, step):
        if axis == "x":
            return {"tp": y * NX + ring(x, step, NX)}
        return {"tp": ring(y, step, NY) * NX + x}

    weights = [
        pltpu.make_async_copy(wg, wgu.at[:, :, pl.ds(0, LANES)], wsem.at[0]),
        pltpu.make_async_copy(wu, wgu.at[:, :, pl.ds(LANES, LANES)], wsem.at[1]),
        pltpu.make_async_copy(wd, wdn, wsem.at[2]),
    ]
    loads = [
        pltpu.make_async_copy(src, dst, wsem.at[3 + i])
        for i, (src, dst) in enumerate(
            ((rout_in, rout), (tok_in, tok), (gw_in, gw), (gain_in, gain))
        )
    ]
    for copy in loads:
        copy.start()

    barrier = pltpu.get_barrier_semaphore()
    peers = [{"ep": ep_at(d, o)} for d in ORDER for o in range(2) if (d, o) != (0, 0)]
    peers += [beside(a, s) for a in ("x", "y") for s in (1, -1, 2)]
    for peer in peers:
        pl.semaphore_signal(barrier, inc=1, device_id=peer, device_id_type=MESH)

    for copy in loads[:3]:
        copy.wait()
    for copy in weights:
        copy.start()
    chosen = rout[...]
    names = lax.broadcasted_iota(jnp.int32, (64, 32), 0)
    hot = [jnp.where(chosen[k : k + 1, :] == names, 1.0, 0.0) for k in range(4)]
    named = hot[0] + hot[1] + hot[2] + hot[3]
    upper = jnp.where(
        lax.broadcasted_iota(jnp.int32, (32, 32), 0) < lax.broadcasted_iota(jnp.int32, (32, 32), 1),
        1.0, 0.0,
    )
    before = jnp.dot(
        named.astype(jnp.bfloat16), upper.astype(jnp.bfloat16), preferred_element_type=jnp.float32
    )
    slots = lax.broadcasted_iota(jnp.int32, (512, 32), 0)
    place = jnp.zeros((512, 32), jnp.float32)
    mix = jnp.zeros((512, 32), jnp.float32)
    for k in range(4):
        rank = jnp.sum(before * hot[k], axis=0, keepdims=True).astype(jnp.int32)
        match = (chosen[k : k + 1, :] * CAP + rank) == slots
        place = place + jnp.where(match, 1.0, 0.0)
        mix = mix + jnp.where(match, gw[k : k + 1, :], 0.0)
    comb[...] = mix
    outgoing[...] = jnp.dot(
        place.astype(jnp.bfloat16), tok[...], preferred_element_type=jnp.float32
    ).astype(jnp.bfloat16).reshape(32, EXP_DEV, CAP, LANES)

    pl.semaphore_wait(barrier, len(peers))

    sends = []

    def send(src, dst, ssem, rsem, device):
        copy = pltpu.make_async_remote_copy(
            src_ref=src, dst_ref=dst, send_sem=ssem, recv_sem=rsem, device_id=device,
            device_id_type=MESH,
        )
        copy.start()
        sends.append(copy)
        return copy

    mine, where = ep // (2 * PER), lax.rem(ep, 2 * PER)
    for d in ORDER:
        for o in range(2):
            target = ep_at(d, o)
            if (d, o) == (0, 0):
                own = outgoing[target]
                for e in range(EXP_DEV):
                    gath[mine, y, x, e, where] = own[e]
                continue
            send(
                outgoing.at[target], gath.at[mine, y, x, :, where],
                zs.at[(d % NZ) * 2 + o], zr.at[ep], {"ep": target},
            )

    live = {}
    first, second = ("x", "y"), ("y", "x")

    def pos(axis):
        return x if axis == "x" else y

    def hop(name, c, h, axis, views):
        stage = ("a1", "a3", "a4", "r1", "r2", "r3").index(name)
        made = []
        for j, step in enumerate((1, -1, 2)[: len(views)]):
            src, dst = views[j]
            idx = ((stage * NC + c) * 2 + h) * 3 + j
            made.append(send(src, dst, rs.at[idx], rr.at[idx], beside(axis, step)))
        live[(name, c, h)] = made

    def landed(name, c, h):
        for copy in live[(name, c, h)]:
            copy.wait_recv()

    def block(c, h, i, j, lo=0, n=ROWS // CAP):
        return gath.at[c, i, j, h, pl.ds(lo, n)]

    def line(ref, c, h, axis, at, lo=0, n=ROWS // CAP):
        if axis == "y":
            return ref.at[c, at, :, h, pl.ds(lo, n)]
        return ref.at[c, :, at, h, pl.ds(lo, n)]

    K2 = HALF // CAP

    def select(c):
        for i in range(2 * PER):
            source = c * 2 * PER + i

            @pl.when(ep != source)
            def _(source=source, i=i):
                pltpu.make_async_remote_copy(
                    src_ref=outgoing.at[source], dst_ref=gath.at[c, y, x, :, i],
                    send_sem=zs.at[0], recv_sem=zr.at[source], device_id={"ep": source},
                    device_id_type=MESH,
                ).wait_recv()

    def a1(c, h):
        view = block(c, h, y, x)
        hop("a1", c, h, first[h], [(view, view)] * 3)

    def a3(c, h):
        landed("a1", c, h)
        a = second[h]
        view = line(gath, c, h, a, pos(a))
        hop("a3", c, h, a, [(view, view)] * 2)

    def a4(c, h):
        landed("a3", c, h)
        a = second[h]
        v0 = line(gath, c, h, a, ring(pos(a), -1, 4), 0, K2)
        v1 = line(gath, c, h, a, ring(pos(a), 1, 4), K2, K2)
        hop("a4", c, h, a, [(v0, v0), (v1, v1)])

    def r1(c, h):
        landed("a4", c, h)
        if (c, h) == WEIGHTS_AT:
            for copy in weights + loads[3:]:
                copy.wait()
        raw = jnp.concatenate(
            [gath[c, i, j, h].reshape(ROWS, LANES) for i in range(NY) for j in range(NX)],
            axis=1,
        )
        wide = raw.astype(jnp.float32)
        ssq = jnp.sum(wide * wide, axis=1, keepdims=True)
        rows = (wide * lax.rsqrt(ssq / D + norm_eps) * gain[...]).astype(jnp.bfloat16)
        both = jnp.dot(rows, wgu[h], preferred_element_type=jnp.float32)
        hidden = activate(both[:, :LANES], both[:, LANES:])
        value = jnp.dot(hidden, wdn[h], preferred_element_type=jnp.float32).astype(jnp.bfloat16)
        for i in range(NY):
            for j in range(NX):
                at = (i * NX + j) * LANES
                part[c, i, j, h] = value[:, at : at + LANES].reshape(ROWS // CAP, CAP, LANES)
        a = second[h]
        far = ring(pos(a), 2, 4)
        hop("r1", c, h, a, [
            (line(part, c, h, a, far, 0, K2), rb1.at[c, h, 0]),
            (line(part, c, h, a, far, K2, K2), rb1.at[c, h, 1]),
        ])

    def add_into(ref_view, other):
        ref_view[...] = (
            ref_view[...].astype(jnp.float32) + other[...].astype(jnp.float32)
        ).astype(jnp.bfloat16)

    def r2(c, h):
        landed("r1", c, h)
        a = second[h]
        ahead, back = ring(pos(a), 1, 4), ring(pos(a), -1, 4)
        add_into(line(part, c, h, a, ahead, 0, K2), rb1.at[c, h, 0])
        add_into(line(part, c, h, a, back, K2, K2), rb1.at[c, h, 1])
        hop("r2", c, h, a, [
            (line(part, c, h, a, ahead), rb2.at[c, h, 0]),
            (line(part, c, h, a, back), rb2.at[c, h, 1]),
        ])

    def r3(c, h):
        landed("r2", c, h)
        a, b = second[h], first[h]
        total = line(part, c, h, a, pos(a))[...].astype(jnp.float32)
        total = total + rb2[c, h, 0].astype(jnp.float32) + rb2[c, h, 1].astype(jnp.float32)
        quart[c, h] = total.astype(jnp.bfloat16)
        hop("r3", c, h, b, [
            (quart.at[c, h, ring(pos(b), step, 4)], rb4.at[c, h, j])
            for j, step in enumerate((1, -1, 2))
        ])

    def fin(c, h):
        landed("r3", c, h)
        total = quart[c, h, pos(first[h])].astype(jnp.float32)
        for j in range(3):
            total = total + rb4[c, h, j].astype(jnp.float32)
        final[c, h] = total.astype(jnp.bfloat16)
        if (c, h) in GOES:
            go_home(c)

    def home(c, i, target):
        return pltpu.make_async_remote_copy(
            src_ref=final.at[c, :, i], dst_ref=ret.at[ep],
            send_sem=hs.at[target], recv_sem=hr.at[ep], device_id={"ep": target},
            device_id_type=MESH,
        )

    def go_home(c):
        for i in range(2 * PER):
            target = c * 2 * PER + i

            @pl.when(ep == target)
            def _(target=target, i=i):
                for e in range(EXP_DEV):
                    ret[target, e] = final[c, e, i]

            @pl.when(ep != target)
            def _(target=target, i=i):
                home(c, i, target).start()

    stages = dict(a1=a1, a3=a3, a4=a4, r1=r1, r2=r2, r3=r3, fin=fin)
    done = set()
    for name, c, h in PLAN:
        if c not in done:
            done.add(c)
            select(c)
        stages[name](c, h)

    for source in range(32):

        @pl.when(ep != source)
        def _(source=source):
            copy = pltpu.make_async_remote_copy(
                src_ref=final.at[source // (2 * PER), :, source % (2 * PER)], dst_ref=ret.at[source],
                send_sem=hs.at[source], recv_sem=hr.at[source], device_id={"ep": source},
                device_id_type=MESH,
            )
            copy.wait_recv()
            copy.wait_send()

    mixed = lax.dot_general(
        comb[...], ret[...].reshape(512, LANES).astype(jnp.float32), (((0,), (0,)), ((), ())),
        preferred_element_type=jnp.float32, precision=lax.Precision.HIGHEST,
    )
    out[...] = mixed.astype(jnp.bfloat16)
    for copy in sends:
        copy.wait_send()


def per_device(tokens, routing, gate_weights, norm_gain, w_gate, w_up, w_down):
    vmem = pl.BlockSpec(memory_space=pltpu.VMEM)
    hbm = pl.BlockSpec(memory_space=pltpu.HBM)
    tiles = ROWS // CAP
    bf = jnp.bfloat16
    hops = 6 * NC * 2 * 3
    return pl.pallas_call(
        kernel,
        out_shape=jax.ShapeDtypeStruct((32, LANES), bf),
        in_specs=[hbm] * 7,
        out_specs=vmem,
        scratch_shapes=[
            pltpu.VMEM((32, LANES), bf),
            pltpu.VMEM((4, 32), jnp.int32),
            pltpu.VMEM((4, 32), jnp.float32),
            pltpu.VMEM((1, D), jnp.float32),
            pltpu.VMEM((32, EXP_DEV, CAP, LANES), bf),
            pltpu.VMEM((NC, NY, NX, EXP_DEV, tiles, CAP, LANES), bf),
            pltpu.VMEM((NC, NY, NX, EXP_DEV, tiles, CAP, LANES), bf),
            pltpu.VMEM((NC, 2, 2, 4, tiles // 2, CAP, LANES), bf),
            pltpu.VMEM((NC, 2, 2, 4, tiles, CAP, LANES), bf),
            pltpu.VMEM((NC, 2, 4, tiles, CAP, LANES), bf),
            pltpu.VMEM((NC, 2, 3, tiles, CAP, LANES), bf),
            pltpu.VMEM((NC, 2, tiles, CAP, LANES), bf),
            pltpu.VMEM((32, EXP_DEV, CAP, LANES), bf),
            pltpu.VMEM((EXP_DEV, D, 2 * LANES), bf),
            pltpu.VMEM((EXP_DEV, LANES, D), bf),
            pltpu.VMEM((512, 32), jnp.float32),
            pltpu.SemaphoreType.DMA((7,)),
            pltpu.SemaphoreType.DMA((32,)),
            pltpu.SemaphoreType.DMA((32,)),
            pltpu.SemaphoreType.DMA((hops,)),
            pltpu.SemaphoreType.DMA((hops,)),
            pltpu.SemaphoreType.DMA((32,)),
            pltpu.SemaphoreType.DMA((32,)),
        ],
        compiler_params=pltpu.CompilerParams(
            collective_id=0, has_side_effects=True, vmem_limit_bytes=67043328
        ),
        name="moe_step",
    )(tokens, routing.T, gate_weights.T, norm_gain.reshape(1, D), w_gate, w_up, w_down)


def solution(mesh):
    placed = (
        P("ep", "tp"),
        P("ep", None),
        P("ep", None),
        P(),
        P("ep", None, "tp"),
        P("ep", None, "tp"),
        P("ep", "tp", None),
    )
    return jax.shard_map(
        per_device, mesh=mesh, in_specs=placed, out_specs=P("ep", "tp"), check_vma=False
    )
```

```python
import functools

import jax
import jax.numpy as jnp
from jax import lax
from jax.experimental import pallas as pl
from jax.experimental.pallas import tpu as pltpu
from jax.sharding import PartitionSpec as P

D = 2048
CAP = 8
NX = 4
NY = 4
NZ = 16
EXP_DEV = 2
LANES = 128
NC = 4
ORDER = (8, -7, 7, -6, 6, -5, 5, -4, 4, -3, 3, -2, 2, -1, 1, 0)
PER = NZ // NC
ROWS = PER * 2 * CAP
HALF = ROWS // 2

PLAN = (
    ("a1", 0, 0),
    ("a1", 0, 1),
    ("a1", 1, 0),
    ("a1", 1, 1),
    ("a3", 0, 0),
    ("a3", 0, 1),
    ("a1", 2, 0),
    ("a1", 2, 1),
    ("a1", 3, 0),
    ("a1", 3, 1),
    ("a3", 1, 0),
    ("a3", 1, 1),
    ("a4", 0, 0),
    ("a4", 0, 1),
    ("a3", 2, 1),
    ("a3", 2, 0),
    ("a3", 3, 1),
    ("a3", 3, 0),
    ("a4", 1, 0),
    ("a4", 1, 1),
    ("r1", 0, 0),
    ("r1", 0, 1),
    ("a4", 2, 0),
    ("a4", 2, 1),
    ("a4", 3, 0),
    ("a4", 3, 1),
    ("r1", 1, 0),
    ("r2", 0, 0),
    ("r1", 1, 1),
    ("r2", 0, 1),
    ("r1", 2, 0),
    ("r1", 2, 1),
    ("r2", 1, 0),
    ("r1", 3, 0),
    ("r2", 1, 1),
    ("r3", 0, 0),
    ("r1", 3, 1),
    ("r3", 0, 1),
    ("r2", 2, 0),
    ("r2", 2, 1),
    ("r3", 1, 0),
    ("r2", 3, 0),
    ("r3", 1, 1),
    ("fin", 0, 1),
    ("fin", 0, 0),
    ("r2", 3, 1),
    ("r3", 2, 0),
    ("r3", 2, 1),
    ("r3", 3, 0),
    ("fin", 1, 0),
    ("fin", 1, 1),
    ("r3", 3, 1),
    ("fin", 2, 0),
    ("fin", 2, 1),
    ("fin", 3, 0),
    ("fin", 3, 1),
)
WEIGHTS_AT = (0, 0)
GOES = ((0, 0), (1, 1), (2, 1), (3, 1))

norm_eps = 1e-06
clamp_limit = 7.0
swish_alpha = 1.702
MESH = pl.DeviceIdType.MESH


def activate(pre_gate, pre_up):
    clamped = jnp.minimum(pre_gate, clamp_limit)
    upper = jnp.clip(pre_up, -clamp_limit, clamp_limit)
    return (clamped * jax.nn.sigmoid(swish_alpha * clamped) * (upper + 1.0)).astype(jnp.bfloat16)


def kernel(
    tok_in, rout_in, gw_in, gain_in, wg, wu, wd, out,
    tok, rout, gw, gain, outgoing, gath, part, rb1, rb2, quart, rb4, final, ret, wgu, wdn, comb,
    wsem, zs, zr, rs, rr, hs, hr,
):
    ep = lax.axis_index("ep")
    tp = lax.axis_index("tp")
    z, core = ep // 2, lax.rem(ep, 2)
    y, x = tp // NX, lax.rem(tp, NX)

    def ring(value, step, size):
        return lax.rem(value + step + size, size)

    def ep_at(dz, other):
        return ring(z, dz, NZ) * 2 + (lax.rem(core + other, 2))

    def beside(axis, step):
        if axis == "x":
            return {"tp": y * NX + ring(x, step, NX)}
        return {"tp": ring(y, step, NY) * NX + x}

    weights = [
        pltpu.make_async_copy(wg, wgu.at[:, :, pl.ds(0, LANES)], wsem.at[0]),
        pltpu.make_async_copy(wu, wgu.at[:, :, pl.ds(LANES, LANES)], wsem.at[1]),
        pltpu.make_async_copy(wd, wdn, wsem.at[2]),
    ]
    loads = [
        pltpu.make_async_copy(src, dst, wsem.at[3 + i])
        for i, (src, dst) in enumerate(
            ((rout_in, rout), (tok_in, tok), (gw_in, gw), (gain_in, gain))
        )
    ]
    for copy in loads:
        copy.start()

    barrier = pltpu.get_barrier_semaphore()
    peers = [{"ep": ep_at(d, o)} for d in ORDER for o in range(2) if (d, o) != (0, 0)]
    peers += [beside(a, s) for a in ("x", "y") for s in (1, -1, 2)]
    for peer in peers:
        pl.semaphore_signal(barrier, inc=1, device_id=peer, device_id_type=MESH)

    for copy in loads[:3]:
        copy.wait()
    for copy in weights:
        copy.start()
    chosen = rout[...]
    names = lax.broadcasted_iota(jnp.int32, (64, 32), 0)
    hot = [jnp.where(chosen[k : k + 1, :] == names, 1.0, 0.0) for k in range(4)]
    named = hot[0] + hot[1] + hot[2] + hot[3]
    upper = jnp.where(
        lax.broadcasted_iota(jnp.int32, (32, 32), 0) < lax.broadcasted_iota(jnp.int32, (32, 32), 1),
        1.0, 0.0,
    )
    before = jnp.dot(
        named.astype(jnp.bfloat16), upper.astype(jnp.bfloat16), preferred_element_type=jnp.float32
    )
    slots = lax.broadcasted_iota(jnp.int32, (512, 32), 0)
    place = jnp.zeros((512, 32), jnp.float32)
    mix = jnp.zeros((512, 32), jnp.float32)
    for k in range(4):
        rank = jnp.sum(before * hot[k], axis=0, keepdims=True).astype(jnp.int32)
        match = (chosen[k : k + 1, :] * CAP + rank) == slots
        place = place + jnp.where(match, 1.0, 0.0)
        mix = mix + jnp.where(match, gw[k : k + 1, :], 0.0)
    mix = mix.T
    for n in range(3):
        term = mix.astype(jnp.bfloat16)
        comb[pl.ds(32 * n, 32), :] = term
        mix = mix - term.astype(jnp.float32)
    outgoing[...] = jnp.dot(
        place.astype(jnp.bfloat16), tok[...], preferred_element_type=jnp.float32
    ).astype(jnp.bfloat16).reshape(32, EXP_DEV, CAP, LANES)

    pl.semaphore_wait(barrier, len(peers))

    sends = []

    def send(src, dst, ssem, rsem, device):
        copy = pltpu.make_async_remote_copy(
            src_ref=src, dst_ref=dst, send_sem=ssem, recv_sem=rsem, device_id=device,
            device_id_type=MESH,
        )
        copy.start()
        sends.append(copy)
        return copy

    mine, where = ep // (2 * PER), lax.rem(ep, 2 * PER)
    for d in ORDER:
        for o in range(2):
            target = ep_at(d, o)
            if (d, o) == (0, 0):
                own = outgoing[target]
                for e in range(EXP_DEV):
                    gath[mine, y, x, e, where] = own[e]
                continue
            send(
                outgoing.at[target], gath.at[mine, y, x, :, where],
                zs.at[(d % NZ) * 2 + o], zr.at[ep], {"ep": target},
            )

    live = {}
    first, second = ("x", "y"), ("y", "x")

    def pos(axis):
        return x if axis == "x" else y

    def hop(name, c, h, axis, views):
        stage = ("a1", "a3", "a4", "r1", "r2", "r3").index(name)
        made = []
        for j, step in enumerate((1, -1, 2)[: len(views)]):
            src, dst = views[j]
            idx = ((stage * NC + c) * 2 + h) * 3 + j
            made.append(send(src, dst, rs.at[idx], rr.at[idx], beside(axis, step)))
        live[(name, c, h)] = made

    def landed(name, c, h):
        for copy in live[(name, c, h)]:
            copy.wait_recv()

    def block(c, h, i, j, lo=0, n=ROWS // CAP):
        return gath.at[c, i, j, h, pl.ds(lo, n)]

    def line(ref, c, h, axis, at, lo=0, n=ROWS // CAP):
        if axis == "y":
            return ref.at[c, at, :, h, pl.ds(lo, n)]
        return ref.at[c, :, at, h, pl.ds(lo, n)]

    K2 = HALF // CAP

    def select(c):
        for i in range(2 * PER):
            source = c * 2 * PER + i

            @pl.when(ep != source)
            def _(source=source, i=i):
                pltpu.make_async_remote_copy(
                    src_ref=outgoing.at[source], dst_ref=gath.at[c, y, x, :, i],
                    send_sem=zs.at[0], recv_sem=zr.at[source], device_id={"ep": source},
                    device_id_type=MESH,
                ).wait_recv()

    def a1(c, h):
        view = block(c, h, y, x)
        hop("a1", c, h, first[h], [(view, view)] * 3)

    def a3(c, h):
        landed("a1", c, h)
        a = second[h]
        view = line(gath, c, h, a, pos(a))
        hop("a3", c, h, a, [(view, view)] * 2)

    def a4(c, h):
        landed("a3", c, h)
        a = second[h]
        v0 = line(gath, c, h, a, ring(pos(a), -1, 4), 0, K2)
        v1 = line(gath, c, h, a, ring(pos(a), 1, 4), K2, K2)
        hop("a4", c, h, a, [(v0, v0), (v1, v1)])

    def r1(c, h):
        landed("a4", c, h)
        if (c, h) == WEIGHTS_AT:
            for copy in weights + loads[3:]:
                copy.wait()
        raw = jnp.concatenate(
            [gath[c, i, j, h].reshape(ROWS, LANES) for i in range(NY) for j in range(NX)],
            axis=1,
        )
        wide = raw.astype(jnp.float32)
        ssq = jnp.sum(wide * wide, axis=1, keepdims=True)
        rows = (wide * lax.rsqrt(ssq / D + norm_eps) * gain[...]).astype(jnp.bfloat16)
        both = jnp.dot(rows, wgu[h], preferred_element_type=jnp.float32)
        hidden = activate(both[:, :LANES], both[:, LANES:])
        value = jnp.dot(hidden, wdn[h], preferred_element_type=jnp.float32).astype(jnp.bfloat16)
        for i in range(NY):
            for j in range(NX):
                at = (i * NX + j) * LANES
                part[c, i, j, h] = value[:, at : at + LANES].reshape(ROWS // CAP, CAP, LANES)
        a = second[h]
        far = ring(pos(a), 2, 4)
        hop("r1", c, h, a, [
            (line(part, c, h, a, far, 0, K2), rb1.at[c, h, 0]),
            (line(part, c, h, a, far, K2, K2), rb1.at[c, h, 1]),
        ])

    def add_into(ref_view, other):
        ref_view[...] = (
            ref_view[...].astype(jnp.float32) + other[...].astype(jnp.float32)
        ).astype(jnp.bfloat16)

    def r2(c, h):
        landed("r1", c, h)
        a = second[h]
        ahead, back = ring(pos(a), 1, 4), ring(pos(a), -1, 4)
        add_into(line(part, c, h, a, ahead, 0, K2), rb1.at[c, h, 0])
        add_into(line(part, c, h, a, back, K2, K2), rb1.at[c, h, 1])
        hop("r2", c, h, a, [
            (line(part, c, h, a, ahead), rb2.at[c, h, 0]),
            (line(part, c, h, a, back), rb2.at[c, h, 1]),
        ])

    def r3(c, h):
        landed("r2", c, h)
        a, b = second[h], first[h]
        total = line(part, c, h, a, pos(a))[...].astype(jnp.float32)
        total = total + rb2[c, h, 0].astype(jnp.float32) + rb2[c, h, 1].astype(jnp.float32)
        quart[c, h] = total.astype(jnp.bfloat16)
        hop("r3", c, h, b, [
            (quart.at[c, h, ring(pos(b), step, 4)], rb4.at[c, h, j])
            for j, step in enumerate((1, -1, 2))
        ])

    def fin(c, h):
        landed("r3", c, h)
        total = quart[c, h, pos(first[h])].astype(jnp.float32)
        for j in range(3):
            total = total + rb4[c, h, j].astype(jnp.float32)
        final[c, h] = total.astype(jnp.bfloat16)
        if (c, h) in GOES:
            go_home(c)

    def home(c, i, target):
        return pltpu.make_async_remote_copy(
            src_ref=final.at[c, :, i], dst_ref=ret.at[ep],
            send_sem=hs.at[target], recv_sem=hr.at[ep], device_id={"ep": target},
            device_id_type=MESH,
        )

    def go_home(c):
        for i in range(2 * PER):
            target = c * 2 * PER + i

            @pl.when(ep == target)
            def _(target=target, i=i):
                for e in range(EXP_DEV):
                    ret[target, e] = final[c, e, i]

            @pl.when(ep != target)
            def _(target=target, i=i):
                home(c, i, target).start()

    stages = dict(a1=a1, a3=a3, a4=a4, r1=r1, r2=r2, r3=r3, fin=fin)
    done = set()
    for name, c, h in PLAN:
        if c not in done:
            done.add(c)
            select(c)
        stages[name](c, h)

    for copy in sends:
        copy.wait_send()

    for source in range(32):

        @pl.when(ep != source)
        def _(source=source):
            copy = pltpu.make_async_remote_copy(
                src_ref=final.at[source // (2 * PER), :, source % (2 * PER)], dst_ref=ret.at[source],
                send_sem=hs.at[source], recv_sem=hr.at[source], device_id={"ep": source},
                device_id_type=MESH,
            )
            copy.wait_recv()
            copy.wait_send()

    terms = jnp.dot(
        comb[...], ret[...].reshape(512, LANES), preferred_element_type=jnp.float32
    )
    out[...] = (terms[:32] + terms[32:64] + terms[64:]).astype(jnp.bfloat16)


def per_device(tokens, routing, gate_weights, norm_gain, w_gate, w_up, w_down):
    vmem = pl.BlockSpec(memory_space=pltpu.VMEM)
    hbm = pl.BlockSpec(memory_space=pltpu.HBM)
    tiles = ROWS // CAP
    bf = jnp.bfloat16
    hops = 6 * NC * 2 * 3
    return pl.pallas_call(
        kernel,
        out_shape=jax.ShapeDtypeStruct((32, LANES), bf),
        in_specs=[hbm] * 7,
        out_specs=vmem,
        scratch_shapes=[
            pltpu.VMEM((32, LANES), bf),
            pltpu.VMEM((4, 32), jnp.int32),
            pltpu.VMEM((4, 32), jnp.float32),
            pltpu.VMEM((1, D), jnp.float32),
            pltpu.VMEM((32, EXP_DEV, CAP, LANES), bf),
            pltpu.VMEM((NC, NY, NX, EXP_DEV, tiles, CAP, LANES), bf),
            pltpu.VMEM((NC, NY, NX, EXP_DEV, tiles, CAP, LANES), bf),
            pltpu.VMEM((NC, 2, 2, 4, tiles // 2, CAP, LANES), bf),
            pltpu.VMEM((NC, 2, 2, 4, tiles, CAP, LANES), bf),
            pltpu.VMEM((NC, 2, 4, tiles, CAP, LANES), bf),
            pltpu.VMEM((NC, 2, 3, tiles, CAP, LANES), bf),
            pltpu.VMEM((NC, 2, tiles, CAP, LANES), bf),
            pltpu.VMEM((32, EXP_DEV, CAP, LANES), bf),
            pltpu.VMEM((EXP_DEV, D, 2 * LANES), bf),
            pltpu.VMEM((EXP_DEV, LANES, D), bf),
            pltpu.VMEM((96, 512), bf),
            pltpu.SemaphoreType.DMA((7,)),
            pltpu.SemaphoreType.DMA((32,)),
            pltpu.SemaphoreType.DMA((32,)),
            pltpu.SemaphoreType.DMA((hops,)),
            pltpu.SemaphoreType.DMA((hops,)),
            pltpu.SemaphoreType.DMA((32,)),
            pltpu.SemaphoreType.DMA((32,)),
        ],
        compiler_params=pltpu.CompilerParams(
            collective_id=0, has_side_effects=True, vmem_limit_bytes=67043328
        ),
        name="moe_step",
    )(tokens, routing.T, gate_weights.T, norm_gain.reshape(1, D), w_gate, w_up, w_down)


def solution(mesh):
    placed = (
        P("ep", "tp"),
        P("ep", None),
        P("ep", None),
        P(),
        P("ep", None, "tp"),
        P("ep", None, "tp"),
        P("ep", "tp", None),
    )
    return jax.shard_map(
        per_device, mesh=mesh, in_specs=placed, out_specs=P("ep", "tp"), check_vma=False
    )
```

```python
import functools

import jax
import jax.numpy as jnp
from jax import lax
from jax.experimental import pallas as pl
from jax.experimental.pallas import tpu as pltpu
from jax.sharding import PartitionSpec as P

D = 2048
CAP = 8
NX = 4
NY = 4
NZ = 16
EXP_DEV = 2
LANES = 128
NC = 4
ORDER = (8, -7, 7, -6, 6, -5, 5, -4, 4, -3, 3, -2, 2, -1, 1, 0)
PER = NZ // NC
ROWS = PER * 2 * CAP
HALF = ROWS // 2

PLAN = (
    ("a1", 0, 0),
    ("a1", 0, 1),
    ("a1", 1, 0),
    ("a1", 1, 1),
    ("a3", 0, 0),
    ("a3", 0, 1),
    ("a1", 2, 0),
    ("a1", 2, 1),
    ("a1", 3, 0),
    ("a1", 3, 1),
    ("a3", 1, 0),
    ("a3", 1, 1),
    ("a4", 0, 0),
    ("a4", 0, 1),
    ("a3", 2, 1),
    ("a3", 2, 0),
    ("a3", 3, 1),
    ("a3", 3, 0),
    ("a4", 1, 0),
    ("a4", 1, 1),
    ("r1", 0, 0),
    ("r1", 0, 1),
    ("a4", 2, 0),
    ("a4", 2, 1),
    ("a4", 3, 0),
    ("a4", 3, 1),
    ("r1", 1, 0),
    ("r2", 0, 0),
    ("r1", 1, 1),
    ("r2", 0, 1),
    ("r1", 2, 0),
    ("r1", 2, 1),
    ("r2", 1, 0),
    ("r1", 3, 0),
    ("r2", 1, 1),
    ("r3", 0, 0),
    ("r1", 3, 1),
    ("r3", 0, 1),
    ("r2", 2, 0),
    ("r2", 2, 1),
    ("r3", 1, 0),
    ("r2", 3, 0),
    ("r3", 1, 1),
    ("fin", 0, 1),
    ("fin", 0, 0),
    ("r2", 3, 1),
    ("r3", 2, 0),
    ("r3", 2, 1),
    ("r3", 3, 0),
    ("fin", 1, 0),
    ("fin", 1, 1),
    ("r3", 3, 1),
    ("fin", 2, 0),
    ("fin", 2, 1),
    ("fin", 3, 0),
    ("fin", 3, 1),
)
WEIGHTS_AT = (0, 0)
GOES = ((0, 0), (1, 1), (2, 1), (3, 1))

norm_eps = 1e-06
clamp_limit = 7.0
swish_alpha = 1.702
MESH = pl.DeviceIdType.MESH


def activate(pre_gate, pre_up):
    clamped = jnp.minimum(pre_gate, clamp_limit)
    upper = jnp.clip(pre_up, -clamp_limit, clamp_limit)
    return (clamped * jax.nn.sigmoid(swish_alpha * clamped) * (upper + 1.0)).astype(jnp.bfloat16)


def kernel(
    tok_in, rout_in, gw_in, gain_in, wg, wu, wd, out,
    tok, rout, gw, gain, outgoing, gath, part, rb1, rb2, quart, rb4, final, ret, wgu, wdn, comb,
    wsem, zs, zr, rs, rr, hs, hr,
):
    ep = lax.axis_index("ep")
    tp = lax.axis_index("tp")
    z, core = ep // 2, lax.rem(ep, 2)
    y, x = tp // NX, lax.rem(tp, NX)

    def ring(value, step, size):
        return lax.rem(value + step + size, size)

    def ep_at(dz, other):
        return ring(z, dz, NZ) * 2 + (lax.rem(core + other, 2))

    def beside(axis, step):
        if axis == "x":
            return {"tp": y * NX + ring(x, step, NX)}
        return {"tp": ring(y, step, NY) * NX + x}

    weights = [
        pltpu.make_async_copy(wg, wgu.at[:, :, pl.ds(0, LANES)], wsem.at[0]),
        pltpu.make_async_copy(wu, wgu.at[:, :, pl.ds(LANES, LANES)], wsem.at[1]),
        pltpu.make_async_copy(wd, wdn, wsem.at[2]),
    ]
    loads = [
        pltpu.make_async_copy(src, dst, wsem.at[3 + i])
        for i, (src, dst) in enumerate(
            ((rout_in, rout), (tok_in, tok), (gw_in, gw), (gain_in, gain))
        )
    ]
    for copy in loads:
        copy.start()

    barrier = pltpu.get_barrier_semaphore()
    peers = [{"ep": ep_at(d, o)} for d in ORDER for o in range(2) if (d, o) != (0, 0)]
    peers += [beside(a, s) for a in ("x", "y") for s in (1, -1, 2)]
    for peer in peers:
        pl.semaphore_signal(barrier, inc=1, device_id=peer, device_id_type=MESH)

    for copy in loads[:3]:
        copy.wait()
    for copy in weights:
        copy.start()
    chosen = rout[...]
    names = lax.broadcasted_iota(jnp.int32, (64, 32), 0)
    hot = [jnp.where(chosen[k : k + 1, :] == names, 1.0, 0.0) for k in range(4)]
    named = hot[0] + hot[1] + hot[2] + hot[3]
    upper = jnp.where(
        lax.broadcasted_iota(jnp.int32, (32, 32), 0) < lax.broadcasted_iota(jnp.int32, (32, 32), 1),
        1.0, 0.0,
    )
    before = jnp.dot(
        named.astype(jnp.bfloat16), upper.astype(jnp.bfloat16), preferred_element_type=jnp.float32
    )
    slots = lax.broadcasted_iota(jnp.int32, (512, 32), 0)
    place = jnp.zeros((512, 32), jnp.float32)
    mix = jnp.zeros((512, 32), jnp.float32)
    for k in range(4):
        rank = jnp.sum(before * hot[k], axis=0, keepdims=True).astype(jnp.int32)
        match = (chosen[k : k + 1, :] * CAP + rank) == slots
        place = place + jnp.where(match, 1.0, 0.0)
        mix = mix + jnp.where(match, gw[k : k + 1, :], 0.0)
    mix = mix.T
    for n in range(3):
        term = mix.astype(jnp.bfloat16)
        comb[pl.ds(32 * n, 32), :] = term
        mix = mix - term.astype(jnp.float32)
    outgoing[...] = jnp.dot(
        place.astype(jnp.bfloat16), tok[...], preferred_element_type=jnp.float32
    ).astype(jnp.bfloat16).reshape(32, EXP_DEV, CAP, LANES)

    pl.semaphore_wait(barrier, len(peers))

    sends = []

    def send(src, dst, ssem, rsem, device):
        copy = pltpu.make_async_remote_copy(
            src_ref=src, dst_ref=dst, send_sem=ssem, recv_sem=rsem, device_id=device,
            device_id_type=MESH,
        )
        copy.start()
        sends.append(copy)
        return copy

    mine, where = ep // (2 * PER), lax.rem(ep, 2 * PER)
    for d in ORDER:
        for o in range(2):
            target = ep_at(d, o)
            if (d, o) == (0, 0):
                own = outgoing[target]
                for e in range(EXP_DEV):
                    gath[mine, y, x, e, where] = own[e]
                continue
            send(
                outgoing.at[target], gath.at[mine, y, x, :, where],
                zs.at[(d % NZ) * 2 + o], zr.at[ep], {"ep": target},
            )

    live = {}
    first, second = ("x", "y"), ("y", "x")

    def pos(axis):
        return x if axis == "x" else y

    def hop(name, c, h, axis, views):
        stage = ("a1", "a3", "a4", "r1", "r2", "r3").index(name)
        made = []
        steps = ((0, 1), (1, -1)) if len(views) == 2 else ((2, 2), (0, 1), (1, -1))
        for j, step in steps:
            src, dst = views[j]
            idx = ((stage * NC + c) * 2 + h) * 3 + j
            made.append(send(src, dst, rs.at[idx], rr.at[idx], beside(axis, step)))
        live[(name, c, h)] = made

    def landed(name, c, h):
        for copy in live[(name, c, h)]:
            copy.wait_recv()

    def block(c, h, i, j, lo=0, n=ROWS // CAP):
        return gath.at[c, i, j, h, pl.ds(lo, n)]

    def line(ref, c, h, axis, at, lo=0, n=ROWS // CAP):
        if axis == "y":
            return ref.at[c, at, :, h, pl.ds(lo, n)]
        return ref.at[c, :, at, h, pl.ds(lo, n)]

    K2 = HALF // CAP

    def select(c):
        for i in range(2 * PER):
            source = c * 2 * PER + i

            @pl.when(ep != source)
            def _(source=source, i=i):
                pltpu.make_async_remote_copy(
                    src_ref=outgoing.at[source], dst_ref=gath.at[c, y, x, :, i],
                    send_sem=zs.at[0], recv_sem=zr.at[source], device_id={"ep": source},
                    device_id_type=MESH,
                ).wait_recv()

    def a1(c, h):
        view = block(c, h, y, x)
        hop("a1", c, h, first[h], [(view, view)] * 3)

    def a3(c, h):
        landed("a1", c, h)
        a = second[h]
        view = line(gath, c, h, a, pos(a))
        hop("a3", c, h, a, [(view, view)] * 2)

    def a4(c, h):
        landed("a3", c, h)
        a = second[h]
        v0 = line(gath, c, h, a, ring(pos(a), -1, 4), 0, K2)
        v1 = line(gath, c, h, a, ring(pos(a), 1, 4), K2, K2)
        hop("a4", c, h, a, [(v0, v0), (v1, v1)])

    def r1(c, h):
        landed("a4", c, h)
        if (c, h) == WEIGHTS_AT:
            for copy in weights + loads[3:]:
                copy.wait()
        raw = jnp.concatenate(
            [gath[c, i, j, h].reshape(ROWS, LANES) for i in range(NY) for j in range(NX)],
            axis=1,
        )
        wide = raw.astype(jnp.float32)
        ssq = jnp.sum(wide * wide, axis=1, keepdims=True)
        rows = (wide * lax.rsqrt(ssq / D + norm_eps) * gain[...]).astype(jnp.bfloat16)
        both = jnp.dot(rows, wgu[h], preferred_element_type=jnp.float32)
        hidden = activate(both[:, :LANES], both[:, LANES:])
        value = jnp.dot(hidden, wdn[h], preferred_element_type=jnp.float32).astype(jnp.bfloat16)
        for i in range(NY):
            for j in range(NX):
                at = (i * NX + j) * LANES
                part[c, i, j, h] = value[:, at : at + LANES].reshape(ROWS // CAP, CAP, LANES)
        a = second[h]
        far = ring(pos(a), 2, 4)
        hop("r1", c, h, a, [
            (line(part, c, h, a, far, 0, K2), rb1.at[c, h, 0]),
            (line(part, c, h, a, far, K2, K2), rb1.at[c, h, 1]),
        ])

    def add_into(ref_view, other):
        ref_view[...] = (
            ref_view[...].astype(jnp.float32) + other[...].astype(jnp.float32)
        ).astype(jnp.bfloat16)

    def r2(c, h):
        landed("r1", c, h)
        a = second[h]
        ahead, back = ring(pos(a), 1, 4), ring(pos(a), -1, 4)
        add_into(line(part, c, h, a, ahead, 0, K2), rb1.at[c, h, 0])
        add_into(line(part, c, h, a, back, K2, K2), rb1.at[c, h, 1])
        hop("r2", c, h, a, [
            (line(part, c, h, a, ahead), rb2.at[c, h, 0]),
            (line(part, c, h, a, back), rb2.at[c, h, 1]),
        ])

    def r3(c, h):
        landed("r2", c, h)
        a, b = second[h], first[h]
        total = line(part, c, h, a, pos(a))[...].astype(jnp.float32)
        total = total + rb2[c, h, 0].astype(jnp.float32) + rb2[c, h, 1].astype(jnp.float32)
        quart[c, h] = total.astype(jnp.bfloat16)
        hop("r3", c, h, b, [
            (quart.at[c, h, ring(pos(b), step, 4)], rb4.at[c, h, j])
            for j, step in enumerate((1, -1, 2))
        ])

    def fin(c, h):
        landed("r3", c, h)
        total = quart[c, h, pos(first[h])].astype(jnp.float32)
        for j in range(3):
            total = total + rb4[c, h, j].astype(jnp.float32)
        final[c, h] = total.astype(jnp.bfloat16)
        if (c, h) in GOES:
            go_home(c)

    def home(c, i, target):
        return pltpu.make_async_remote_copy(
            src_ref=final.at[c, :, i], dst_ref=ret.at[ep],
            send_sem=hs.at[target], recv_sem=hr.at[ep], device_id={"ep": target},
            device_id_type=MESH,
        )

    def go_home(c):
        for i in range(2 * PER):
            target = c * 2 * PER + i

            @pl.when(ep == target)
            def _(target=target, i=i):
                for e in range(EXP_DEV):
                    ret[target, e] = final[c, e, i]

            @pl.when(ep != target)
            def _(target=target, i=i):
                home(c, i, target).start()

    stages = dict(a1=a1, a3=a3, a4=a4, r1=r1, r2=r2, r3=r3, fin=fin)
    done = set()
    for name, c, h in PLAN:
        if c not in done:
            done.add(c)
            select(c)
        stages[name](c, h)

    for copy in sends:
        copy.wait_send()

    for source in range(32):

        @pl.when(ep != source)
        def _(source=source):
            copy = pltpu.make_async_remote_copy(
                src_ref=final.at[source // (2 * PER), :, source % (2 * PER)], dst_ref=ret.at[source],
                send_sem=hs.at[source], recv_sem=hr.at[source], device_id={"ep": source},
                device_id_type=MESH,
            )
            copy.wait_recv()
            copy.wait_send()

    terms = jnp.dot(
        comb[...], ret[...].reshape(512, LANES), preferred_element_type=jnp.float32
    )
    out[...] = (terms[:32] + terms[32:64] + terms[64:]).astype(jnp.bfloat16)


def per_device(tokens, routing, gate_weights, norm_gain, w_gate, w_up, w_down):
    vmem = pl.BlockSpec(memory_space=pltpu.VMEM)
    hbm = pl.BlockSpec(memory_space=pltpu.HBM)
    tiles = ROWS // CAP
    bf = jnp.bfloat16
    hops = 6 * NC * 2 * 3
    return pl.pallas_call(
        kernel,
        out_shape=jax.ShapeDtypeStruct((32, LANES), bf),
        in_specs=[hbm] * 7,
        out_specs=vmem,
        scratch_shapes=[
            pltpu.VMEM((32, LANES), bf),
            pltpu.VMEM((4, 32), jnp.int32),
            pltpu.VMEM((4, 32), jnp.float32),
            pltpu.VMEM((1, D), jnp.float32),
            pltpu.VMEM((32, EXP_DEV, CAP, LANES), bf),
            pltpu.VMEM((NC, NY, NX, EXP_DEV, tiles, CAP, LANES), bf),
            pltpu.VMEM((NC, NY, NX, EXP_DEV, tiles, CAP, LANES), bf),
            pltpu.VMEM((NC, 2, 2, 4, tiles // 2, CAP, LANES), bf),
            pltpu.VMEM((NC, 2, 2, 4, tiles, CAP, LANES), bf),
            pltpu.VMEM((NC, 2, 4, tiles, CAP, LANES), bf),
            pltpu.VMEM((NC, 2, 3, tiles, CAP, LANES), bf),
            pltpu.VMEM((NC, 2, tiles, CAP, LANES), bf),
            pltpu.VMEM((32, EXP_DEV, CAP, LANES), bf),
            pltpu.VMEM((EXP_DEV, D, 2 * LANES), bf),
            pltpu.VMEM((EXP_DEV, LANES, D), bf),
            pltpu.VMEM((96, 512), bf),
            pltpu.SemaphoreType.DMA((7,)),
            pltpu.SemaphoreType.DMA((32,)),
            pltpu.SemaphoreType.DMA((32,)),
            pltpu.SemaphoreType.DMA((hops,)),
            pltpu.SemaphoreType.DMA((hops,)),
            pltpu.SemaphoreType.DMA((32,)),
            pltpu.SemaphoreType.DMA((32,)),
        ],
        compiler_params=pltpu.CompilerParams(
            collective_id=0, has_side_effects=True, vmem_limit_bytes=67043328
        ),
        name="moe_step",
    )(tokens, routing.T, gate_weights.T, norm_gain.reshape(1, D), w_gate, w_up, w_down)


def solution(mesh):
    placed = (
        P("ep", "tp"),
        P("ep", None),
        P("ep", None),
        P(),
        P("ep", None, "tp"),
        P("ep", None, "tp"),
        P("ep", "tp", None),
    )
    return jax.shard_map(
        per_device, mesh=mesh, in_specs=placed, out_specs=P("ep", "tp"), check_vma=False
    )
```
